32 devices in a mesh: ep: 8 (over z, x), tp: 4 (over y, core).
Axes of the slice: x: 2, y: 2, z: 4, core: 2. Of those that a mesh axis runs over, the one named last changes fastest.
Arguments:
- x_path: bfloat16 [8192, 2048], P('ep', 'tp'), may hold values from -6 to 6
- gate_path: bfloat16 [8192, 2048], P('ep', 'tp'), may hold values from -6 to 6
- conv_taps: float32 [4, 2048], P(None, 'tp'), may hold values from -3 to 3
- decay_gate_w: bfloat16 [2, 16, 128, 128], P(None, 'tp'), may hold values from -0.5 to 0.5
- input_gate_w: bfloat16 [2, 16, 128, 128], P(None, 'tp'), may hold values from -0.5 to 0.5
- decay_rate: float32 [2, 2048], P(None, 'tp'), may hold values from 0 to 1, as said below
- decay_shift: float32 [8192, 16], P('ep', 'tp'), may hold values from -1 to 0, as said below
- expert_in: bfloat16 [512, 2048], P('ep'), may hold values from -6 to 6
- norm_gain: float32 [2048], replicated, may hold values from 0.1 to 1.9
- routes: int32 [512, 2], P('ep'), may hold values from 0 to 7, all different within a row; in each aligned block of 16 rows (0 to 15, 16 to 31, ...) at most 8 rows name the same one
- route_scores: float32 [512, 2], P('ep'), may hold values from 0.1 to 1
- gate_weight: bfloat16 [8, 2048, 4096], P('ep', None, 'tp'), may hold values from -0.125 to 0.125
- up_weight: bfloat16 [8, 2048, 4096], P('ep', None, 'tp'), may hold values from -0.125 to 0.125
- down_weight: bfloat16 [8, 4096, 2048], P('ep', 'tp'), may hold values from -0.09375 to 0.09375
Outputs:
- recurrent_out: bfloat16 [8192, 2048], P('ep', 'tp')
- expert_out: bfloat16 [512, 2048], P(('ep', 'tp'))
The draws below stay inside these ranges and needn't reach their ends.
Inputs may be any that keep to these rules, and one draw needn't show every extreme that they name: `routes`: in each aligned block of 16 rows no expert is named by more than 8 rows, and in some block some expert is named by exactly 8 rows; each row names 2 different experts. `decay_rate`: positive rates. `decay_shift`: never positive.
All inputs are finite; a program needn't handle non-finite values.
Results may differ from the reference program's by a relative error of at most 0.019.
Values may be sent and summed in bfloat16 or wider, within the bound.
A program may use at most 128 MiB of HBM per device.

```python
import math
import jax
import jax.numpy as jnp
import numpy as np
from jax import lax

D = 2048
RECURRENT_HEADS = 16
HEAD_DIM = 128
WIDTH = 2048
FF = 4096
FF_DEV = 1024
TOP_K = 2
EXPERTS = 8
MIX_ROWS = 1024
MIXER_TOKENS = 8192
EXP_ROWS = 16
EXP_TOKENS = 512
CAPACITY = 8
N_TP = 4


def draw_decay_rate(key, part):
    pick_key, fast_key, slow_key = jax.random.split(key, 3)
    fast_share = 0.5
    is_fast = jax.random.uniform(pick_key, (2, RECURRENT_HEADS, 1), jnp.float32) < fast_share
    forget_span = float(min(40, MIX_ROWS // 2))
    fast_rate = jnp.exp(jax.random.uniform(fast_key, (2, RECURRENT_HEADS, HEAD_DIM), jnp.float32, math.log(0.5), math.log(1.5))) / (4.0 * forget_span)
    slow_rate = jnp.exp(jax.random.uniform(slow_key, (2, RECURRENT_HEADS, HEAD_DIM), jnp.float32, math.log(0.5), math.log(2.0))) * (0.12 / MIXER_TOKENS)
    return jnp.where(is_fast, fast_rate, slow_rate).reshape(2, RECURRENT_HEADS * HEAD_DIM)


def draw_decay_shift(key, part):
    block_key, location_random_key, depth_random_key = jax.random.split(key, 3)
    block_count = MIXER_TOKENS // MIX_ROWS
    per_block = -jax.random.uniform(block_key, (block_count, 1, RECURRENT_HEADS), jnp.float32, 0.2, 2.0) * (0.3 / MIXER_TOKENS)
    baseline_level = jnp.broadcast_to(per_block, (block_count, MIX_ROWS, RECURRENT_HEADS)).reshape(MIXER_TOKENS, RECURRENT_HEADS)
    spike_locations = jax.random.randint(location_random_key, (2, RECURRENT_HEADS), 0, MIXER_TOKENS)
    spike_depths = jnp.log(jax.random.uniform(depth_random_key, (2, RECURRENT_HEADS), jnp.float32, 0.5, 0.8))
    token_positions = jnp.arange(MIXER_TOKENS, dtype=jnp.int32)[:, None]
    initial_spike = jnp.where(token_positions == spike_locations[0][None, :], spike_depths[0][None, :], 0.0)
    following_spike = jnp.where(token_positions == spike_locations[1][None, :], spike_depths[1][None, :], 0.0)
    return baseline_level + initial_spike + following_spike


def steps_of(key, extent, cuts, least, top_value):
    factor_of, own = 1.0, jax.random.fold_in(key, 6)
    for dim, shards_of in cuts:
        draws = jnp.exp(jax.random.uniform(jax.random.fold_in(own, dim), (shards_of,), jnp.float32, least / len(cuts), top_value / len(cuts)))
        factor_of = factor_of * jnp.repeat(draws, extent[dim] // shards_of).reshape([-1 if axis == dim else 1 for axis in range(len(extent))])
    return factor_of


def routed_block(key, own, number, rows, number_of, top, bound, slope):
    sequence = jax.random.permutation(key, number_of)
    crowded, usual = load_shares(number_of, rows * top, bound, slope, True), load_shares(number_of, rows * top, bound, slope, False)
    places = jnp.arange(number_of)

    def named(lengths, offset_by):
        used = int((lengths > 0).sum())
        fixed = max(1, used // 4)
        passed = fixed + (places - fixed + offset_by * (used - fixed)) % max(1, number_of - fixed)
        return jnp.zeros((number_of,), jnp.int32).at[sequence[jnp.where(places < fixed, places, passed)]].set(jnp.asarray(lengths, jnp.int32))

    lengths = jnp.where(number % 4 == 0, named(crowded, number // 4), named(usual, number - number // 4 - 1))
    mixed = jax.random.permutation(jax.random.fold_in(own, 3), number_of)
    giver, taker = mixed[0:number_of // 2 * 2:2], mixed[1:number_of // 2 * 2:2]
    slack = jnp.minimum(lengths[giver] - 1, bound - lengths[taker]) // 2
    slack = jnp.where((giver == sequence[0]) | (taker == sequence[0]) | (lengths[taker] == 0), 0, jnp.maximum(slack, 0))
    passed = jax.random.randint(jax.random.fold_in(own, 4), (number_of // 2,), 0, 1 << 20) % (slack + 1)
    lengths = lengths.at[giver].add(-passed).at[taker].add(passed)
    labels = jnp.searchsorted(jnp.cumsum(lengths), jnp.arange(rows * top), side="right").astype(jnp.int32)
    listing = labels.reshape(top, rows).T
    listing = listing[jax.random.permutation(jax.random.fold_in(own, 1), rows)]
    offset_by = jax.random.randint(jax.random.fold_in(own, 2), (rows, 1), 0, top)
    return jnp.take_along_axis(listing, (jnp.arange(top)[None, :] + offset_by) % top, axis=1)


def load_shares(count, total, bound, lean, full):
    weights = [(1 << 20) // math.isqrt(rank ** lean) + 1 for rank in range(1, count + 1)]
    largest = bound if full else min(bound, max(-(-total // count), total * weights[0] // sum(weights)))
    least = 1 if total - largest >= count - 1 else 0
    holding, surplus = [largest] + [least] * (count - 1), total - largest - least * (count - 1)
    while surplus > 0:
        movable = [i for i in range(1, count) if holding[i] < largest] or [i for i in range(1, count) if holding[i] < bound]
        mass, remaining = sum([weights[i] for i in movable]), surplus
        for i in movable:
            addition = min(bound - holding[i], max(1, remaining * weights[i] // mass), surplus)
            holding[i] = holding[i] + addition
            surplus = surplus - addition
    return np.array(holding)


def noise(own_key, dims, width, reach, shards=(), kind=jnp.bfloat16):
    values = width * jax.random.normal(own_key, dims, jnp.float32)
    if shards:
        values = values * steps_of(own_key, dims, shards, -0.22, 0.18)
    return jnp.clip(values, -reach, reach).astype(kind)


def setup_inputs(seed: int = 0) -> dict:
    splits = jax.random.split(jax.random.key(seed), 15)
    x_path = noise(splits[0], (MIXER_TOKENS, WIDTH), 1.0, 6.0, ((0, 8), (1, 4)))
    gate_path = noise(splits[1], (MIXER_TOKENS, WIDTH), 1.0, 6.0, ((0, 8), (1, 4)))
    conv_taps = noise(splits[2], (4, WIDTH), 0.5, 3.0, ((1, 4),), jnp.float32)
    decay_gate_w = noise(splits[3], (2, RECURRENT_HEADS, HEAD_DIM, HEAD_DIM), HEAD_DIM ** -0.5, 0.5, ((1, 4),))
    input_gate_w = noise(splits[4], (2, RECURRENT_HEADS, HEAD_DIM, HEAD_DIM), HEAD_DIM ** -0.5, 0.5, ((1, 4),))
    decay_rate = draw_decay_rate(jax.random.fold_in(splits[14], 71), 0)
    decay_shift = draw_decay_shift(jax.random.fold_in(splits[14], 71), 0)
    expert_in = noise(splits[7], (EXP_TOKENS, D), 1.0, 6.0, ((0, 8),))
    norm_gain = jnp.clip(1.0 + 0.18 * jax.random.normal(splits[8], (D,), jnp.float32), 0.1, 1.9)
    routes_keys = jax.random.split(jax.random.fold_in(splits[9], 1), EXP_TOKENS // EXP_ROWS)
    routes_turns = jax.random.permutation(jax.random.fold_in(splits[9], 3), EXP_TOKENS // EXP_ROWS)
    routes = jax.vmap(lambda own, number: routed_block(jax.random.fold_in(splits[9], 2), own, number, EXP_ROWS, EXPERTS, TOP_K, CAPACITY, 1))(routes_keys, routes_turns).reshape((EXP_TOKENS, TOP_K))
    route_scores = jnp.clip(jnp.exp(math.log(1.0) - 2.3025851 * jax.random.uniform(splits[10], (EXP_TOKENS, TOP_K), jnp.float32) ** steps_of(splits[10], (EXP_TOKENS, TOP_K), ((0, 8),), -0.2, 0.2)), 0.1, 1.0)
    gate_weight = noise(splits[11], (EXPERTS, D, FF), D ** -0.5, 0.125, ((0, 8), (2, 4)))
    up_weight = noise(splits[12], (EXPERTS, D, FF), D ** -0.5, 0.125, ((0, 8), (2, 4)))
    down_weight = noise(splits[13], (EXPERTS, FF, D), FF ** -0.5, 0.09375, ((0, 8), (1, 4)))
    return {"x_path": x_path, "gate_path": gate_path, "conv_taps": conv_taps, "decay_gate_w": decay_gate_w, "input_gate_w": input_gate_w, "decay_rate": decay_rate, "decay_shift": decay_shift, "expert_in": expert_in, "norm_gain": norm_gain, "routes": routes, "route_scores": route_scores, "gate_weight": gate_weight, "up_weight": up_weight, "down_weight": down_weight}


EPSILON = 1e-06

def link_pairs(earlier, later):
    return (earlier[0] * later[0], later[0] * earlier[1] + later[1])

def block_gates(conv_block, weights):
    length = conv_block.shape[0]
    grouped = conv_block.astype(jnp.float32).reshape(length, RECURRENT_HEADS, HEAD_DIM)
    preact = jnp.einsum('thi,hij->thj', grouped, weights.astype(jnp.float32))
    return jax.nn.sigmoid(preact).reshape(length, WIDTH)

def chain_states(conv_out, decay_weights, input_weights, rate, shift):
    length = conv_out.shape[0]
    span_rows = math.gcd(length, 512)
    span_count = length // span_rows

    def advance(carry, inputs):
        conv_block, shift_block = inputs
        decay_gate = block_gates(conv_block, decay_weights)
        input_gate = block_gates(conv_block, input_weights)
        log_decay = -8.0 * decay_gate * rate + jnp.repeat(shift_block, HEAD_DIM, axis=1)
        drive = jnp.sqrt(-jnp.expm1(2.0 * log_decay)) * input_gate * conv_block.astype(jnp.float32)
        decay = jnp.exp(log_decay)
        drive = drive.at[0].add(decay[0] * carry)
        states = lax.associative_scan(link_pairs, (decay, drive), axis=0)[1]
        return (states[-1], states)
    initial = jnp.zeros((WIDTH,), jnp.float32)
    blocks_in = (conv_out.reshape(span_count, span_rows, WIDTH), shift.reshape(span_count, span_rows, RECURRENT_HEADS))
    _, states = lax.scan(advance, initial, blocks_in)
    return states.reshape(length, WIDTH)

def recurrence_half(x_path, gate_path, conv_taps, decay_gate_w, input_gate_w, decay_rate, decay_shift):
    length = x_path.shape[0]
    padded = jnp.pad(x_path.astype(jnp.float32), ((2, 1), (0, 0)))
    conv_sum = jnp.zeros((length, WIDTH), jnp.float32)
    for offset in range(4):
        conv_sum = conv_sum + padded[offset:offset + length] * conv_taps[offset]
    conv_out = conv_sum.astype(jnp.bfloat16)
    forward_state = chain_states(conv_out, decay_gate_w[0], input_gate_w[0], decay_rate[0], decay_shift)
    backward_state = chain_states(conv_out[::-1], decay_gate_w[1], input_gate_w[1], decay_rate[1], decay_shift[::-1])[::-1]
    gated = jax.nn.gelu(gate_path.astype(jnp.float32))
    return ((forward_state + backward_state) * gated).astype(jnp.bfloat16)

def slot_ranks(routes):
    tokens = routes.shape[0]
    block_count = tokens // EXP_ROWS
    flattened = routes.reshape(block_count, EXP_ROWS * TOP_K)
    onehot = (flattened[:, :, None] == jnp.arange(EXPERTS, dtype=jnp.int32)[None, None, :]).astype(jnp.int32)
    earlier = lax.optimization_barrier(jnp.sum((jnp.cumsum(onehot, axis=1) - onehot) * onehot, axis=2))
    return earlier.reshape(tokens, TOP_K).astype(jnp.int32)

def expert_half(expert_in, norm_gain, routes, route_scores, gate_weight, up_weight, down_weight):
    tokens = expert_in.shape[0]
    block_count = tokens // EXP_ROWS
    wide_in = expert_in.astype(jnp.float32)
    scale = lax.rsqrt(lax.optimization_barrier(jnp.mean(wide_in * wide_in, axis=1, keepdims=True)) + EPSILON)
    normed = (wide_in * scale * norm_gain).astype(jnp.bfloat16)
    ranks = slot_ranks(routes)
    block_of = (jnp.arange(tokens, dtype=jnp.int32) // EXP_ROWS)[:, None]
    columns = (block_of * CAPACITY + ranks).astype(jnp.int32)
    token_ids = jnp.broadcast_to(jnp.arange(tokens, dtype=jnp.int32)[:, None], routes.shape)
    table = jnp.full((EXPERTS, block_count * CAPACITY), tokens, jnp.int32)
    table = table.at[routes, columns].set(token_ids)
    padded = jnp.concatenate([normed, jnp.zeros((1, D), jnp.bfloat16)], axis=0)

    def one_expert(inputs):
        row_index, gate_mat, up_mat, down_mat = inputs
        picked_rows = padded[row_index]
        gate_pre = jnp.dot(picked_rows, gate_mat, preferred_element_type=jnp.float32)
        up_pre = jnp.dot(picked_rows, up_mat, preferred_element_type=jnp.float32)
        hidden = (jax.nn.silu(gate_pre) * up_pre).astype(jnp.bfloat16)
        grouped = hidden.reshape(-1, N_TP, FF_DEV).astype(jnp.float32)
        down_groups = down_mat.reshape(N_TP, FF_DEV, D).astype(jnp.float32)
        partial_value = jnp.einsum('ngf,gfd->gnd', grouped, down_groups)
        rounded = lax.optimization_barrier(partial_value.astype(jnp.bfloat16)).astype(jnp.float32)
        return lax.optimization_barrier(jnp.sum(rounded, axis=0)).astype(jnp.bfloat16)
    outputs = lax.map(one_expert, (table, gate_weight, up_weight, down_weight))
    chosen = outputs[routes, columns]
    shares = route_scores / lax.optimization_barrier(jnp.sum(route_scores, axis=1, keepdims=True))
    return lax.optimization_barrier(jnp.sum(chosen.astype(jnp.float32) * shares[:, :, None], axis=1)).astype(jnp.bfloat16)

def reference(x_path, gate_path, conv_taps, decay_gate_w, input_gate_w, decay_rate, decay_shift, expert_in, norm_gain, routes, route_scores, gate_weight, up_weight, down_weight):
    recurrent_out = recurrence_half(x_path, gate_path, conv_taps, decay_gate_w, input_gate_w, decay_rate, decay_shift)
    expert_out = expert_half(expert_in, norm_gain, routes, route_scores, gate_weight, up_weight, down_weight)
    return (recurrent_out, expert_out)
```

```python
import functools

import jax
import jax.numpy as jnp
from jax import lax
from jax.experimental import pallas as pl
from jax.experimental.pallas import tpu as pltpu
from jax.sharding import PartitionSpec as P

TOP_K = 2
EPSILON = 1e-06
SUB = 8
LANES = 128
EDGE = 16
STEPS = 16
LOG2E = 1.4426950408889634
F32 = jnp.float32
BF16 = jnp.bfloat16
MESH = pl.DeviceIdType.MESH


def remote(src, dst, send, recv, where):
    return pltpu.make_async_remote_copy(
        src_ref=src, dst_ref=dst, send_sem=send, recv_sem=recv, device_id=where, device_id_type=MESH
    )


def kernel(
    n_ep, n_tp, capacity,
    x_ref, gate_hbm, taps_ref, dgw_ref, igw_ref, rate_ref, shift_ref, ein_ref, gain_ref,
    routes_ref, scores_ref, gw_hbm, uw_hbm, dw_hbm,
    rec_hbm, exp_ref,
    xs, yb, af, bf, ab, bb, seg, carry, gathered, halo, gate_v, out_v,
    gw, uw, dw, normed, places, snd, rcv, hid, part, prcv, ret, retrcv, retf,
    local_sem, halo_send, halo_recv, dis_send, dis_recv, sum_send, sum_recv,
    part_send, part_recv, ret_send, ret_recv,
):
    me = lax.axis_index("ep")
    tp = lax.axis_index("tp")
    rows, width = x_ref.shape
    heads = width // LANES
    span = rows // SUB
    tokens, model = ein_ref.shape
    exit_rows = tokens // n_tp
    per_expert = n_tp * capacity
    slots = n_ep * per_expert
    block_slots = n_ep * capacity
    ff = gw_hbm.shape[2]

    loads = [
        pltpu.make_async_copy(gw_hbm.at[0], gw, local_sem.at[0]),
        pltpu.make_async_copy(uw_hbm.at[0], uw, local_sem.at[1]),
        pltpu.make_async_copy(dw_hbm.at[0], dw, local_sem.at[2]),
        pltpu.make_async_copy(gate_hbm, gate_v, local_sem.at[3]),
    ]
    for load in loads:
        load.start()

    barrier = pltpu.get_barrier_semaphore()
    for d in range(1, n_ep):
        pl.semaphore_signal(barrier, inc=1, device_id={"ep": lax.rem(me + d, n_ep)}, device_id_type=MESH)
    for d in range(1, n_tp):
        pl.semaphore_signal(barrier, inc=1, device_id={"tp": lax.rem(tp + d, n_tp)}, device_id_type=MESH)
    pl.semaphore_wait(barrier, n_ep + n_tp - 2)

    up = remote(
        x_ref.at[pl.ds(rows - EDGE, EDGE)], halo.at[0], halo_send.at[0], halo_recv.at[0],
        {"ep": lax.rem(me + 1, n_ep)},
    )
    down = remote(
        x_ref.at[pl.ds(0, EDGE)], halo.at[1], halo_send.at[1], halo_recv.at[1],
        {"ep": lax.rem(me + n_ep - 1, n_ep)},
    )

    @pl.when(me < n_ep - 1)
    def _():
        up.start()

    @pl.when(me > 0)
    def _():
        down.start()

    wide = ein_ref[...].astype(F32)
    scale = lax.rsqrt(jnp.mean(wide * wide, axis=1, keepdims=True) + EPSILON)
    normed[...] = (wide * scale * gain_ref[...]).astype(BF16)
    expert_ids = lax.broadcasted_iota(jnp.int32, (tokens, n_ep), 1)
    first = routes_ref[:, 0:1] == expert_ids
    second = routes_ref[:, 1:2] == expert_ids
    member = (first | second).astype(BF16)
    row_id = lax.broadcasted_iota(jnp.int32, (tokens, tokens), 0)
    col_id = lax.broadcasted_iota(jnp.int32, (tokens, tokens), 1)
    before = (col_id < row_id) & (col_id // exit_rows == row_id // exit_rows)
    ranks = jnp.dot(before.astype(BF16), member, preferred_element_type=F32)
    rank_first = jnp.sum(jnp.where(first, ranks, 0.0), axis=1, keepdims=True).astype(jnp.int32)
    rank_second = jnp.sum(jnp.where(second, ranks, 0.0), axis=1, keepdims=True).astype(jnp.int32)
    places[:, 0:1] = routes_ref[:, 0:1] * capacity + rank_first
    places[:, 1:2] = routes_ref[:, 1:2] * capacity + rank_second
    token_block = lax.broadcasted_iota(jnp.int32, (tokens, 1), 0) // exit_rows
    slot_first = routes_ref[:, 0:1] * per_expert + token_block * capacity + rank_first
    slot_second = routes_ref[:, 1:2] * per_expert + token_block * capacity + rank_second
    slot_ids = lax.broadcasted_iota(jnp.int32, (tokens, slots), 1)
    selector = ((slot_first == slot_ids) | (slot_second == slot_ids)).astype(F32)
    selector = selector.T.astype(BF16)
    for e in range(n_ep):
        snd[e] = jnp.dot(
            selector[e * per_expert : (e + 1) * per_expert], normed[...], preferred_element_type=F32
        ).astype(BF16)
    dispatch = []
    for d in range(1, n_ep):
        peer = lax.rem(me + d, n_ep)
        copy = remote(snd.at[peer], rcv.at[me], dis_send.at[d], dis_recv.at[d], {"ep": peer})
        copy.start()
        dispatch.append(copy)
    rcv_own = pltpu.make_async_copy(snd.at[me], rcv.at[me], local_sem.at[4])
    rcv_own.start()

    def widen(i, c):
        r = pl.multiple_of(i * LANES, LANES)
        for h in range(heads):
            xs[h, pl.ds(SUB + r, LANES), :] = x_ref[
                pl.ds(r, LANES), h * LANES : (h + 1) * LANES
            ].astype(F32)
        return c

    lax.fori_loop(0, rows // LANES, widen, 0)

    @pl.when(me == 0)
    def _():
        halo[0] = jnp.zeros((EDGE, width), BF16)

    @pl.when(me == n_ep - 1)
    def _():
        halo[1] = jnp.zeros((EDGE, width), BF16)

    @pl.when(me > 0)
    def _():
        up.wait_recv()

    @pl.when(me < n_ep - 1)
    def _():
        down.wait_recv()

    lower = halo[0].astype(F32)
    upper = halo[1].astype(F32)
    for h in range(heads):
        lanes = slice(h * LANES, (h + 1) * LANES)
        xs[h, 0:SUB, :] = lower[EDGE - SUB : EDGE, lanes]
        xs[h, SUB + rows : 2 * SUB + rows, :] = upper[0:SUB, lanes]

    ones = jnp.ones((SUB, LANES), F32)
    zeros = jnp.zeros((SUB, LANES), F32)
    for h in range(heads):
        lanes = slice(h * LANES, (h + 1) * LANES)
        taps = [taps_ref[k : k + 1, lanes] for k in range(4)]
        weights = jnp.concatenate(
            [dgw_ref[0, h], dgw_ref[1, h], igw_ref[0, h], igw_ref[1, h]], axis=1
        )
        rates = [rate_ref[d : d + 1, lanes] * (-8.0) for d in range(2)]

        def chunk(c, state, h=h, taps=taps, weights=weights, rates=rates):
            total_f, end_f, total_b, end_b = state
            s0 = c * STEPS
            window = [
                xs[h, pl.ds(SUB - 2 + s0 + i, SUB, stride=span), :] for i in range(STEPS + 3)
            ]
            conv = []
            for i in range(STEPS):
                total = window[i] * taps[0]
                for k in range(1, 4):
                    total = total + window[i + k] * taps[k]
                conv.append(total)
            conv = jnp.concatenate(conv, axis=0).astype(BF16)
            pre = jnp.dot(conv, weights, preferred_element_type=F32)
            conv = conv.astype(F32)
            shift = jnp.concatenate(
                [
                    jnp.broadcast_to(
                        shift_ref[pl.ds(s0 + i, SUB, stride=span), :][:, h : h + 1], (SUB, LANES)
                    )
                    for i in range(STEPS)
                ],
                axis=0,
            )
            place = pl.ds(pl.multiple_of(s0 * SUB, STEPS * SUB), STEPS * SUB)
            pairs = []
            for d, (a_ref, b_ref) in enumerate(((af, bf), (ab, bb))):
                gate = 1.0 / (1.0 + jnp.exp(-pre[:, d * LANES : (d + 1) * LANES]))
                log_decay = gate * rates[d] + shift
                decay = jnp.exp(log_decay)
                x2 = 2.0 * log_decay
                series = -x2 * (1.0 + x2 * (0.5 + x2 * (1.0 / 6.0 + x2 * (1.0 / 24.0))))
                square = jnp.where(x2 > -0.1, series, 1.0 - decay * decay)
                root = jnp.where(square > 0.0, square * lax.rsqrt(square), 0.0)
                half = 0.5 * pre[:, (2 + d) * LANES : (3 + d) * LANES]
                drive = root * (0.5 + 0.5 * jnp.tanh(half)) * conv
                a_ref[h, place, :] = decay
                b_ref[h, place, :] = drive
                pairs.append((decay, drive))
            for i in range(STEPS):
                part_rows = slice(i * SUB, (i + 1) * SUB)
                a, b = pairs[0][0][part_rows], pairs[0][1][part_rows]
                end_f = a * end_f + b
                total_f = total_f * a
                a, b = pairs[1][0][part_rows], pairs[1][1][part_rows]
                end_b = end_b + total_b * b
                total_b = total_b * a
            return total_f, end_f, total_b, end_b

        state = lax.fori_loop(0, span // STEPS, chunk, (ones, zeros, ones, zeros))
        for i in range(4):
            seg[i, :, lanes] = state[i]

    one_row = jnp.ones((1, width), F32)
    zero_row = jnp.zeros((1, width), F32)
    total_f, end_f, total_b, end_b = one_row, zero_row, one_row, zero_row
    for k in range(SUB):
        end_f = seg[0, k : k + 1, :] * end_f + seg[1, k : k + 1, :]
        total_f = total_f * seg[0, k : k + 1, :]
        end_b = end_b + total_b * seg[3, k : k + 1, :]
        total_b = total_b * seg[2, k : k + 1, :]
    gathered[me, 0:1, :] = total_f
    gathered[me, 1:2, :] = end_f
    gathered[me, 2:3, :] = total_b
    gathered[me, 3:4, :] = end_b
    gathered[me, 4:8, :] = jnp.zeros((4, width), F32)
    sums = []
    for d in range(1, n_ep):
        peer = lax.rem(me + d, n_ep)
        copy = remote(gathered.at[me], gathered.at[me], sum_send.at[d], sum_recv.at[d], {"ep": peer})
        copy.start()
        sums.append(copy)

    rcv_own.wait()
    for copy in dispatch:
        copy.wait()
    for load in loads[:3]:
        load.wait()
    arrived = rcv.reshape(slots, model)
    tile = min(256, ff)

    def project(n, c):
        cols = pl.ds(pl.multiple_of(n * tile, tile), tile)
        gate_pre = jnp.dot(arrived[...], gw[:, cols], preferred_element_type=F32)
        up_pre = jnp.dot(arrived[...], uw[:, cols], preferred_element_type=F32)
        hid[:, cols] = (gate_pre / (1.0 + jnp.exp(-gate_pre)) * up_pre).astype(BF16)
        return c

    lax.fori_loop(0, ff // tile, project, 0)
    partials = []
    for d in list(range(1, n_tp)) + [0]:
        peer = lax.rem(tp + d, n_tp)
        out_row = lax.broadcasted_iota(jnp.int32, (block_slots, slots), 0)
        in_row = lax.broadcasted_iota(jnp.int32, (block_slots, slots), 1)
        source = (out_row // capacity) * per_expert + peer * capacity + out_row % capacity
        pick = (source == in_row).astype(BF16)
        picked = jnp.dot(pick, hid[...], preferred_element_type=F32).astype(BF16)
        value = jnp.dot(picked, dw[...], preferred_element_type=F32).astype(BF16)
        if d == 0:
            prcv[0] = value
        else:
            part[d] = value
            copy = remote(part.at[d], prcv.at[d], part_send.at[d], part_recv.at[d], {"tp": peer})
            copy.start()
            partials.append(copy)

    for copy in sums:
        copy.wait()
    carry_f, carry_b = zero_row, zero_row
    for j in range(n_ep):
        carry_f = jnp.where(j < me, gathered[j, 0:1, :] * carry_f + gathered[j, 1:2, :], carry_f)
    for j in range(n_ep - 1, -1, -1):
        carry_b = jnp.where(j > me, gathered[j, 2:3, :] * carry_b + gathered[j, 3:4, :], carry_b)
    for k in range(SUB):
        carry[0, k : k + 1, :] = carry_f
        carry_f = seg[0, k : k + 1, :] * carry_f + seg[1, k : k + 1, :]
    for k in range(SUB - 1, -1, -1):
        carry[1, k : k + 1, :] = carry_b
        carry_b = seg[2, k : k + 1, :] * carry_b + seg[3, k : k + 1, :]

    def advance(c, state):
        state = list(state)
        for i in range(SUB):
            s = c * SUB + i
            r = span - 1 - s
            here = pl.ds(pl.multiple_of(s * SUB, SUB), SUB)
            there = pl.ds(pl.multiple_of(r * SUB, SUB), SUB)
            for h in range(heads):
                state[h] = af[h, here, :] * state[h] + bf[h, here, :]
                xs[h, pl.ds(s, SUB, stride=span), :] = state[h]
                g = heads + h
                state[g] = ab[h, there, :] * state[g] + bb[h, there, :]
                yb[h, pl.ds(r, SUB, stride=span), :] = state[g]
        return tuple(state)

    start = [carry[d, :, h * LANES : (h + 1) * LANES] for d in range(2) for h in range(heads)]
    lax.fori_loop(0, span // SUB, advance, tuple(start))
    loads[3].wait()
    block = 64

    def finish(i, c):
        here = pl.ds(pl.multiple_of(i * block, block), block)
        for h in range(heads):
            lanes = slice(h * LANES, (h + 1) * LANES)
            g = gate_v[here, lanes].astype(F32)
            inner = 0.7978845608028654 * (g + 0.044715 * (g * g * g))
            gated = g * (0.5 * (1.0 + jnp.tanh(inner)))
            out_v[here, lanes] = ((xs[h, here, :] + yb[h, here, :]) * gated).astype(BF16)
        return c

    lax.fori_loop(0, rows // block, finish, 0)
    store = pltpu.make_async_copy(out_v, rec_hbm, local_sem.at[5])
    store.start()

    for copy in partials:
        copy.wait()
    summed = prcv[0].astype(F32)
    for d in range(1, n_tp):
        summed = summed + prcv[d].astype(F32)
    for e in range(n_ep):
        ret[e] = summed[e * capacity : (e + 1) * capacity].astype(BF16)
    backs = []
    for d in range(1, n_ep):
        peer = lax.rem(me + d, n_ep)
        copy = remote(ret.at[peer], retrcv.at[me], ret_send.at[d], ret_recv.at[d], {"ep": peer})
        copy.start()
        backs.append(copy)
    retrcv[me] = ret[me]
    for copy in backs:
        copy.wait()
    for e in range(n_ep):
        retf[e * capacity : (e + 1) * capacity, :] = retrcv[e].astype(F32)
    returned = retf[...].astype(BF16)
    own = pl.ds(pl.multiple_of(tp * exit_rows, exit_rows), exit_rows)
    scores = scores_ref[own, :]
    shares = scores / jnp.sum(scores, axis=1, keepdims=True)
    ids = lax.broadcasted_iota(jnp.int32, (exit_rows, block_slots), 1)
    total = jnp.zeros((exit_rows, model), F32)
    for k in range(TOP_K):
        pick = (places[own, k : k + 1] == ids).astype(BF16)
        total = total + shares[:, k : k + 1] * jnp.dot(pick, returned, preferred_element_type=F32)
    exp_ref[...] = total.astype(BF16)

    @pl.when(me < n_ep - 1)
    def _():
        up.wait_send()

    @pl.when(me > 0)
    def _():
        down.wait_send()

    store.wait()


def local(
    x_path, gate_path, conv_taps, decay_gate_w, input_gate_w, decay_rate, decay_shift, expert_in,
    norm_gain, routes, route_scores, gate_weight, up_weight, down_weight,
):
    n_ep, n_tp = lax.axis_size("ep"), lax.axis_size("tp")
    rows, width = x_path.shape
    heads = width // LANES
    tokens, model = expert_in.shape
    ff = gate_weight.shape[2]
    exit_rows = tokens // n_tp
    capacity = max(2, 2 * exit_rows * TOP_K // n_ep)
    per_expert = n_tp * capacity
    block_slots = n_ep * capacity
    vmem = pl.BlockSpec(memory_space=pltpu.VMEM)
    hbm = pl.BlockSpec(memory_space=pl.ANY)
    pair = pltpu.VMEM((heads, rows, LANES), F32)
    dma = pltpu.SemaphoreType.DMA
    return pl.pallas_call(
        functools.partial(kernel, n_ep, n_tp, capacity),
        out_shape=(
            jax.ShapeDtypeStruct((rows, width), BF16),
            jax.ShapeDtypeStruct((exit_rows, model), BF16),
        ),
        in_specs=[vmem, hbm] + [vmem] * 9 + [hbm] * 3,
        out_specs=(hbm, vmem),
        scratch_shapes=[
            pltpu.VMEM((heads, rows + 2 * SUB, LANES), F32),
            pair, pair, pair, pair, pair,
            pltpu.VMEM((4, SUB, width), F32),
            pltpu.VMEM((2, SUB, width), F32),
            pltpu.VMEM((n_ep, SUB, width), F32),
            pltpu.VMEM((2, EDGE, width), BF16),
            pltpu.VMEM((rows, width), BF16),
            pltpu.VMEM((rows, width), BF16),
            pltpu.VMEM((model, ff), BF16),
            pltpu.VMEM((model, ff), BF16),
            pltpu.VMEM((ff, model), BF16),
            pltpu.VMEM((tokens, model), BF16),
            pltpu.VMEM((tokens, TOP_K), jnp.int32),
            pltpu.VMEM((n_ep, per_expert, model), BF16),
            pltpu.VMEM((n_ep, per_expert, model), BF16),
            pltpu.VMEM((n_ep * per_expert, ff), BF16),
            pltpu.VMEM((n_tp, block_slots, model), BF16),
            pltpu.VMEM((n_tp, block_slots, model), BF16),
            pltpu.VMEM((n_ep, capacity, model), BF16),
            pltpu.VMEM((n_ep, capacity, model), BF16),
            pltpu.VMEM((block_slots, model), F32),
            dma((6,)), dma((2,)), dma((2,)), dma((n_ep,)), dma((n_ep,)), dma((n_ep,)), dma((n_ep,)),
            dma((n_tp,)), dma((n_tp,)), dma((n_ep,)), dma((n_ep,)),
        ],
        compiler_params=pltpu.CompilerParams(
            collective_id=0, has_side_effects=True, vmem_limit_bytes=62 * 1024 * 1024
        ),
        name="layer",
    )(
        x_path, gate_path, conv_taps, decay_gate_w, input_gate_w, decay_rate, decay_shift,
        expert_in, norm_gain.reshape(1, model), routes, route_scores,
        gate_weight, up_weight, down_weight,
    )


def solution(mesh):
    in_specs = (
        P("ep", "tp"),
        P("ep", "tp"),
        P(None, "tp"),
        P(None, "tp", None, None),
        P(None, "tp", None, None),
        P(None, "tp"),
        P("ep", "tp"),
        P("ep", None),
        P(),
        P("ep", None),
        P("ep", None),
        P("ep", None, "tp"),
        P("ep", None, "tp"),
        P("ep", "tp", None),
    )
    out_specs = (P("ep", "tp"), P(("ep", "tp"), None))
    return jax.shard_map(local, mesh=mesh, in_specs=in_specs, out_specs=out_specs, check_vma=False)
```

```python
import functools

import jax
import jax.numpy as jnp
from jax import lax
from jax.experimental import pallas as pl
from jax.experimental.pallas import tpu as pltpu
from jax.sharding import PartitionSpec as P

TOP_K = 2
EPSILON = 1e-06
SUB = 8
LANES = 128
EDGE = 16
STEPS = 16
LOG2E = 1.4426950408889634
F32 = jnp.float32
BF16 = jnp.bfloat16
MESH = pl.DeviceIdType.MESH
PIECES = 2
SHARE_AT = (2, 3)
RELAY_AT = (4, 4)


def remote(src, dst, send, recv, where):
    return pltpu.make_async_remote_copy(
        src_ref=src, dst_ref=dst, send_sem=send, recv_sem=recv, device_id=where, device_id_type=MESH
    )


def kernel(
    n_ep, n_tp, capacity,
    x_ref, gate_hbm, taps_ref, dgw_ref, igw_ref, rate_ref, shift_ref, ein_ref, gain_ref,
    routes_ref, scores_ref, gw_hbm, uw_hbm, dw_hbm,
    rec_hbm, exp_ref,
    xs, yb, af, bf, ab, bb, seg, carry, gathered, halo, gate_v, out_v,
    gw, uw, dw, normed, meta, shift_seg, snd, got, stage, rcv, hid, part, pairs_in, mixed, across,
    ret, retrcv,
    local_sem, halo_send, halo_recv, dis_send, dis_recv, row_send, row_recv, fwd_send, fwd_recv,
    pair_send, pair_recv, far_send, far_recv, sum_send, sum_recv, ret_send, ret_recv,
):
    me = lax.axis_index("ep")
    tp = lax.axis_index("tp")
    rows, width = x_ref.shape
    heads = width // LANES
    span = rows // SUB
    tokens, model = ein_ref.shape
    exit_rows = tokens // n_tp
    block_slots = n_ep * capacity
    core, n_y = lax.rem(tp, 2), n_tp // 2
    y = tp // 2
    partner = y * 2 + 1 - core
    far_ys = [lax.rem(y + d, n_y) for d in range(1, n_y)]
    ff = gw_hbm.shape[2]
    wide_piece = model // PIECES
    pieces = [slice(q * wide_piece, (q + 1) * wide_piece) for q in range(PIECES)]

    loads = [
        pltpu.make_async_copy(gw_hbm.at[0], gw, local_sem.at[0]),
        pltpu.make_async_copy(uw_hbm.at[0], uw, local_sem.at[1]),
        pltpu.make_async_copy(dw_hbm.at[0], dw, local_sem.at[2]),
        pltpu.make_async_copy(gate_hbm, gate_v, local_sem.at[3]),
    ]
    for load in loads:
        load.start()

    barrier = pltpu.get_barrier_semaphore()
    for d in range(1, n_ep):
        pl.semaphore_signal(barrier, inc=1, device_id={"ep": lax.rem(me + d, n_ep)}, device_id_type=MESH)
    for d in range(1, n_tp):
        pl.semaphore_signal(barrier, inc=1, device_id={"tp": lax.rem(tp + d, n_tp)}, device_id_type=MESH)
    pl.semaphore_wait(barrier, n_ep + n_tp - 2)

    up = remote(
        x_ref.at[pl.ds(rows - EDGE, EDGE)], halo.at[0], halo_send.at[0], halo_recv.at[0],
        {"ep": lax.rem(me + 1, n_ep)},
    )
    down = remote(
        x_ref.at[pl.ds(0, EDGE)], halo.at[1], halo_send.at[1], halo_recv.at[1],
        {"ep": lax.rem(me + n_ep - 1, n_ep)},
    )

    @pl.when(me < n_ep - 1)
    def _():
        up.start()

    @pl.when(me > 0)
    def _():
        down.start()

    wide = ein_ref[...].astype(F32)
    scale = lax.rsqrt(jnp.mean(wide * wide, axis=1, keepdims=True) + EPSILON)
    normed[...] = (wide * scale * gain_ref[...]).astype(BF16)
    first_route, second_route = routes_ref[0:1, :], routes_ref[1:2, :]
    expert_ids = lax.broadcasted_iota(jnp.int32, (n_ep, tokens), 0)
    first = first_route == expert_ids
    second = second_route == expert_ids
    member = (first | second).astype(BF16)
    row_id = lax.broadcasted_iota(jnp.int32, (tokens, tokens), 0)
    col_id = lax.broadcasted_iota(jnp.int32, (tokens, tokens), 1)
    before = (row_id < col_id) & (row_id // exit_rows == col_id // exit_rows)
    ranks = jnp.dot(member, before.astype(BF16), preferred_element_type=F32)
    rank_first = jnp.sum(jnp.where(first, ranks, 0.0), axis=0, keepdims=True).astype(jnp.int32)
    rank_second = jnp.sum(jnp.where(second, ranks, 0.0), axis=0, keepdims=True).astype(jnp.int32)
    slot_first = first_route * capacity + rank_first
    slot_second = second_route * capacity + rank_second
    scores = scores_ref[...]
    shares = scores / (scores[0:1] + scores[1:2])
    meta[...] = jnp.concatenate(
        [slot_first.astype(F32), slot_second.astype(F32), shares, jnp.zeros((4, tokens), F32)], axis=0
    ).T
    is_own = lax.broadcasted_iota(jnp.int32, (1, tokens), 1) // exit_rows == tp
    slot_ids = lax.broadcasted_iota(jnp.int32, (block_slots, tokens), 0)
    selector = ((slot_first == slot_ids) | (slot_second == slot_ids)) & is_own
    stage[...] = jnp.dot(selector.astype(BF16), normed[...], preferred_element_type=F32)
    for e in range(n_ep):
        snd[e] = stage[e * capacity : (e + 1) * capacity, :].astype(BF16)
    peer_order = list(range(1, n_ep))
    dispatch = []
    for q, cols in enumerate(pieces):
        copies = []
        for d in peer_order:
            peer = lax.rem(me + d, n_ep)
            copy = remote(
                snd.at[peer, :, cols], got.at[me, :, cols], dis_send.at[d, q], dis_recv.at[d, q],
                {"ep": peer},
            )
            copy.start()
            copies.append(copy)
        dispatch.append(copies)
    got[me] = snd[me]
    rows_sent, forwarded = {}, []

    def share_rows(q):
        cols = pieces[q]
        for copy in dispatch[q]:
            copy.wait()
        for e in range(n_ep):
            stage[e * capacity : (e + 1) * capacity, cols] = got[e, :, cols].astype(F32)
        rcv[tp, :, cols] = stage[:, cols].astype(BF16)
        own_rows = rcv.at[tp, :, cols]
        rows_sent[q] = []
        for d in range(n_y):
            there = far_ys[d] * 2 + core if d < n_y - 1 else partner
            copy = remote(own_rows, own_rows, row_send.at[d, q], row_recv.at[d, q], {"tp": there})
            copy.start()
            rows_sent[q].append(copy)

    def forward_rows(q):
        forwarded.append(rows_sent[q][-1])
        for d in range(1, n_y):
            rows_sent[q][d - 1].wait()
            rows_far = rcv.at[lax.rem(y - d + n_y, n_y) * 2 + core, :, pieces[q]]
            copy = remote(rows_far, rows_far, fwd_send.at[d, q], fwd_recv.at[d, q], {"tp": partner})
            copy.start()
            forwarded.append(copy)

    for h in range(heads):
        for k in range(SUB):
            shift_seg[h, k : k + 1, :] = shift_ref[h : h + 1, k * span : (k + 1) * span]

    def widen(i, c):
        r = pl.multiple_of(i * LANES, LANES)
        for h in range(heads):
            xs[h, pl.ds(SUB + r, LANES), :] = x_ref[
                pl.ds(r, LANES), h * LANES : (h + 1) * LANES
            ].astype(F32)
        return c

    lax.fori_loop(0, rows // LANES, widen, 0)

    @pl.when(me == 0)
    def _():
        halo[0] = jnp.zeros((EDGE, width), BF16)

    @pl.when(me == n_ep - 1)
    def _():
        halo[1] = jnp.zeros((EDGE, width), BF16)

    @pl.when(me > 0)
    def _():
        up.wait_recv()

    @pl.when(me < n_ep - 1)
    def _():
        down.wait_recv()

    lower = halo[0].astype(F32)
    upper = halo[1].astype(F32)
    for h in range(heads):
        lanes = slice(h * LANES, (h + 1) * LANES)
        xs[h, 0:SUB, :] = lower[EDGE - SUB : EDGE, lanes]
        xs[h, SUB + rows : 2 * SUB + rows, :] = upper[0:SUB, lanes]

    relays = []
    for q in range(PIECES):
        relays.append((SHARE_AT[q] * heads // 4, share_rows, q))
        relays.append((RELAY_AT[q] * heads // 4, forward_rows, q))
    relays.sort(key=lambda relay: relay[0])
    ones = jnp.ones((SUB, LANES), F32)
    zeros = jnp.zeros((SUB, LANES), F32)
    for h in range(heads):
        for at, act, q in relays:
            if h == at:
                act(q)
        lanes = slice(h * LANES, (h + 1) * LANES)
        taps = [taps_ref[k : k + 1, lanes] for k in range(4)]
        weights = jnp.concatenate(
            [dgw_ref[0, h], dgw_ref[1, h], igw_ref[0, h], igw_ref[1, h]], axis=1
        )
        rates = [rate_ref[d : d + 1, lanes] * (-8.0) for d in range(2)]

        def chunk(c, state, h=h, taps=taps, weights=weights, rates=rates):
            total_f, end_f, total_b, end_b = state
            s0 = c * STEPS
            window = [
                xs[h, pl.ds(SUB - 2 + s0 + i, SUB, stride=span), :] for i in range(STEPS + 3)
            ]
            conv = []
            for i in range(STEPS):
                total = window[i] * taps[0]
                for k in range(1, 4):
                    total = total + window[i + k] * taps[k]
                conv.append(total)
            conv = jnp.concatenate(conv, axis=0).astype(BF16)
            pre = jnp.dot(conv, weights, preferred_element_type=F32)
            conv = conv.astype(F32)
            rolled = pltpu.roll(shift_seg[h], lax.rem(span - s0, span), 1)
            shift = jnp.concatenate(
                [
                    jnp.broadcast_to(
                        rolled[:, i : i + 1], (SUB, LANES)
                    )
                    for i in range(STEPS)
                ],
                axis=0,
            )
            place = pl.ds(pl.multiple_of(s0 * SUB, STEPS * SUB), STEPS * SUB)
            pairs = []
            for d, (a_ref, b_ref) in enumerate(((af, bf), (ab, bb))):
                gate = 1.0 / (1.0 + jnp.exp(-pre[:, d * LANES : (d + 1) * LANES]))
                log_decay = gate * rates[d] + shift
                decay = jnp.exp(log_decay)
                x2 = 2.0 * log_decay
                series = -x2 * (1.0 + x2 * (0.5 + x2 * (1.0 / 6.0 + x2 * (1.0 / 24.0))))
                square = jnp.where(x2 > -0.1, series, 1.0 - decay * decay)
                root = jnp.where(square > 0.0, square * lax.rsqrt(square), 0.0)
                half = 0.5 * pre[:, (2 + d) * LANES : (3 + d) * LANES]
                drive = root * (0.5 + 0.5 * jnp.tanh(half)) * conv
                a_ref[h, place, :] = decay
                b_ref[h, place, :] = drive
                pairs.append((decay, drive))
            for i in range(STEPS):
                part_rows = slice(i * SUB, (i + 1) * SUB)
                a, b = pairs[0][0][part_rows], pairs[0][1][part_rows]
                end_f = a * end_f + b
                total_f = total_f * a
                a, b = pairs[1][0][part_rows], pairs[1][1][part_rows]
                end_b = end_b + total_b * b
                total_b = total_b * a
            return total_f, end_f, total_b, end_b

        state = lax.fori_loop(0, span // STEPS, chunk, (ones, zeros, ones, zeros))
        for i in range(4):
            seg[i, :, lanes] = state[i]

    one_row = jnp.ones((1, width), F32)
    zero_row = jnp.zeros((1, width), F32)
    total_f, end_f, total_b, end_b = one_row, zero_row, one_row, zero_row
    for k in range(SUB):
        end_f = seg[0, k : k + 1, :] * end_f + seg[1, k : k + 1, :]
        total_f = total_f * seg[0, k : k + 1, :]
        end_b = end_b + total_b * seg[3, k : k + 1, :]
        total_b = total_b * seg[2, k : k + 1, :]
    gathered[me, 0:1, :] = total_f
    gathered[me, 1:2, :] = end_f
    gathered[me, 2:3, :] = total_b
    gathered[me, 3:4, :] = end_b
    gathered[me, 4:8, :] = jnp.zeros((4, width), F32)
    sums = []
    for d in range(1, n_ep):
        peer = lax.rem(me + d, n_ep)
        copy = remote(gathered.at[me], gathered.at[me], sum_send.at[d], sum_recv.at[d], {"ep": peer})
        copy.start()
        sums.append(copy)

    for at, act, q in relays:
        if at >= heads:
            act(q)
    for copy in forwarded:
        copy.wait()
    for load in loads[:3]:
        load.wait()
    arrived = rcv.reshape(n_tp * block_slots, model)
    tile = min(256, ff)

    def project(n, c):
        cols = pl.ds(pl.multiple_of(n * tile, tile), tile)
        gate_pre = jnp.dot(arrived[...], gw[:, cols], preferred_element_type=F32)
        up_pre = jnp.dot(arrived[...], uw[:, cols], preferred_element_type=F32)
        hid[:, cols] = (gate_pre / (1.0 + jnp.exp(-gate_pre)) * up_pre).astype(BF16)
        return c

    lax.fori_loop(0, ff // tile, project, 0)

    def reduce_part(block, cols):
        here = pl.ds(pl.multiple_of(block * block_slots, block_slots), block_slots)
        return jnp.dot(hid[here, :], dw[:, cols], preferred_element_type=F32).astype(BF16)

    pair_copies, far_copies = {}, {}
    for q, cols in enumerate(pieces):
        for d in list(range(1, n_y)) + [0]:
            part[d, :, cols] = reduce_part(lax.rem(y + d, n_y) * 2 + 1 - core, cols)
            copy = remote(
                part.at[d, :, cols], pairs_in.at[d, :, cols], pair_send.at[d, q], pair_recv.at[d, q],
                {"tp": partner},
            )
            copy.start()
            pair_copies[d, q] = copy
        for d in range(1, n_y):
            far = lax.rem(y + d, n_y)
            value = reduce_part(far * 2 + core, cols)
            pair_copies[d, q].wait()
            mixed[d, :, cols] = (value.astype(F32) + pairs_in[d, :, cols].astype(F32)).astype(BF16)
            copy = remote(
                mixed.at[d, :, cols], across.at[d, :, cols], far_send.at[d, q], far_recv.at[d, q],
                {"tp": far * 2 + core},
            )
            copy.start()
            far_copies[d, q] = copy
        across[0, :, cols] = reduce_part(tp, cols)

    for copy in sums:
        copy.wait()
    carry_f, carry_b = zero_row, zero_row
    for j in range(n_ep):
        carry_f = jnp.where(j < me, gathered[j, 0:1, :] * carry_f + gathered[j, 1:2, :], carry_f)
    for j in range(n_ep - 1, -1, -1):
        carry_b = jnp.where(j > me, gathered[j, 2:3, :] * carry_b + gathered[j, 3:4, :], carry_b)
    for k in range(SUB):
        carry[0, k : k + 1, :] = carry_f
        carry_f = seg[0, k : k + 1, :] * carry_f + seg[1, k : k + 1, :]
    for k in range(SUB - 1, -1, -1):
        carry[1, k : k + 1, :] = carry_b
        carry_b = seg[2, k : k + 1, :] * carry_b + seg[3, k : k + 1, :]

    def advance(c, state):
        state = list(state)
        for i in range(SUB):
            s = c * SUB + i
            r = span - 1 - s
            here = pl.ds(pl.multiple_of(s * SUB, SUB), SUB)
            there = pl.ds(pl.multiple_of(r * SUB, SUB), SUB)
            for h in range(heads):
                state[h] = af[h, here, :] * state[h] + bf[h, here, :]
                xs[h, pl.ds(s, SUB, stride=span), :] = state[h]
                g = heads + h
                state[g] = ab[h, there, :] * state[g] + bb[h, there, :]
                yb[h, pl.ds(r, SUB, stride=span), :] = state[g]
        return tuple(state)

    start = [carry[d, :, h * LANES : (h + 1) * LANES] for d in range(2) for h in range(heads)]
    lax.fori_loop(0, span // SUB, advance, tuple(start))
    backs = []
    for q, cols in enumerate(pieces):
        pair_copies[0, q].wait()
        summed = across[0, :, cols].astype(F32) + pairs_in[0, :, cols].astype(F32)
        for d in range(1, n_y):
            far_copies[d, q].wait()
            summed = summed + across[d, :, cols].astype(F32)
        stage[:, cols] = summed
        for e in range(n_ep):
            ret[e, :, cols] = stage[e * capacity : (e + 1) * capacity, cols].astype(BF16)
        copies = []
        for d in peer_order:
            peer = lax.rem(me + d, n_ep)
            copy = remote(
                ret.at[peer, :, cols], retrcv.at[me, :, cols], ret_send.at[d, q], ret_recv.at[d, q],
                {"ep": peer},
            )
            copy.start()
            copies.append(copy)
        backs.append(copies)
    retrcv[me] = ret[me]
    loads[3].wait()
    block = 64

    def finish(i, c):
        here = pl.ds(pl.multiple_of(i * block, block), block)
        for h in range(heads):
            lanes = slice(h * LANES, (h + 1) * LANES)
            g = gate_v[here, lanes].astype(F32)
            inner = 0.7978845608028654 * (g + 0.044715 * (g * g * g))
            gated = g * (0.5 * (1.0 + jnp.tanh(inner)))
            out_v[here, lanes] = ((xs[h, here, :] + yb[h, here, :]) * gated).astype(BF16)
        return c

    lax.fori_loop(0, rows // block, finish, 0)
    store = pltpu.make_async_copy(out_v, rec_hbm, local_sem.at[5])
    store.start()

    own = pl.ds(pl.multiple_of(tp * exit_rows, exit_rows), exit_rows)
    own_meta = meta[own, :]
    ids = lax.broadcasted_iota(jnp.int32, (exit_rows, block_slots), 1)
    picks = [(own_meta[:, k : k + 1].astype(jnp.int32) == ids).astype(BF16) for k in range(TOP_K)]
    for q, cols in enumerate(pieces):
        for copy in backs[q]:
            copy.wait()
        for e in range(n_ep):
            stage[e * capacity : (e + 1) * capacity, cols] = retrcv[e, :, cols].astype(F32)
        returned = stage[:, cols].astype(BF16)
        total = jnp.zeros((exit_rows, wide_piece), F32)
        for k in range(TOP_K):
            chosen = jnp.dot(picks[k], returned, preferred_element_type=F32)
            total = total + own_meta[:, TOP_K + k : TOP_K + k + 1] * chosen
        exp_ref[:, cols] = total.astype(BF16)

    @pl.when(me < n_ep - 1)
    def _():
        up.wait_send()

    @pl.when(me > 0)
    def _():
        down.wait_send()

    store.wait()


def hand_over_kernel(rec_ref, exp_ref, rec_out, exp_out, rec_v, exp_v, in_sem, out_sem):
    rows = rec_ref.shape[0]
    step = rows // PIECES
    routes = [
        (rec_ref.at[pl.ds(i * step, step)], rec_v.at[pl.ds(i * step, step)], rec_out.at[pl.ds(i * step, step)])
        for i in range(PIECES)
    ] + [(exp_ref, exp_v, exp_out)]
    ins = [pltpu.make_async_copy(a, b, in_sem.at[i]) for i, (a, b, _) in enumerate(routes)]
    outs = [pltpu.make_async_copy(b, c, out_sem.at[i]) for i, (_, b, c) in enumerate(routes)]
    for copy in ins:
        copy.start()
    for copy, then in zip(ins, outs):
        copy.wait()
        then.start()
    for copy in outs:
        copy.wait()


def hand_over(recurrent, expert):
    hbm = pl.BlockSpec(memory_space=pl.ANY)
    shapes = [jax.ShapeDtypeStruct(a.shape, a.dtype) for a in (recurrent, expert)]
    return pl.pallas_call(
        hand_over_kernel,
        out_shape=tuple(shapes),
        in_specs=[hbm, hbm],
        out_specs=(hbm, hbm),
        scratch_shapes=[pltpu.VMEM(a.shape, a.dtype) for a in shapes]
        + [pltpu.SemaphoreType.DMA((PIECES + 1,))] * 2,
        name="hand_over",
    )(recurrent, expert)


def local(
    x_path, gate_path, conv_taps, decay_gate_w, input_gate_w, decay_rate, decay_shift, expert_in,
    norm_gain, routes, route_scores, gate_weight, up_weight, down_weight,
):
    n_ep, n_tp = lax.axis_size("ep"), lax.axis_size("tp")
    rows, width = x_path.shape
    heads = width // LANES
    tokens, model = expert_in.shape
    ff = gate_weight.shape[2]
    exit_rows = tokens // n_tp
    capacity = max(2, 2 * exit_rows * TOP_K // n_ep)
    block_slots = n_ep * capacity
    n_y = n_tp // 2
    rows_of_tp = pltpu.VMEM((n_tp, block_slots, model), BF16)
    rows_of_y = pltpu.VMEM((n_y, block_slots, model), BF16)
    vmem = pl.BlockSpec(memory_space=pltpu.VMEM)
    hbm = pl.BlockSpec(memory_space=pl.ANY)
    pair = pltpu.VMEM((heads, rows, LANES), F32)
    dma = pltpu.SemaphoreType.DMA
    over_ep, over_y = dma((n_ep, PIECES)), dma((n_y, PIECES))
    recurrent, expert = pl.pallas_call(
        functools.partial(kernel, n_ep, n_tp, capacity),
        out_shape=(
            jax.ShapeDtypeStruct((rows, width), BF16),
            jax.ShapeDtypeStruct((exit_rows, model), BF16),
        ),
        in_specs=[vmem, hbm] + [vmem] * 9 + [hbm] * 3,
        out_specs=(hbm, vmem),
        scratch_shapes=[
            pltpu.VMEM((heads, rows + 2 * SUB, LANES), F32),
            pair, pair, pair, pair, pair,
            pltpu.VMEM((4, SUB, width), F32),
            pltpu.VMEM((2, SUB, width), F32),
            pltpu.VMEM((n_ep, SUB, width), F32),
            pltpu.VMEM((2, EDGE, width), BF16),
            pltpu.VMEM((rows, width), BF16),
            pltpu.VMEM((rows, width), BF16),
            pltpu.VMEM((model, ff), BF16),
            pltpu.VMEM((model, ff), BF16),
            pltpu.VMEM((ff, model), BF16),
            pltpu.VMEM((tokens, model), BF16),
            pltpu.VMEM((tokens, SUB), F32),
            pltpu.VMEM((heads, SUB, rows // SUB), F32),
            pltpu.VMEM((n_ep, capacity, model), BF16),
            pltpu.VMEM((n_ep, capacity, model), BF16),
            pltpu.VMEM((block_slots, model), F32),
            rows_of_tp,
            pltpu.VMEM((n_tp * block_slots, ff), BF16),
            rows_of_y, rows_of_y, rows_of_y, rows_of_y,
            pltpu.VMEM((n_ep, capacity, model), BF16),
            pltpu.VMEM((n_ep, capacity, model), BF16),
            dma((6,)), dma((2,)), dma((2,)), over_ep, over_ep, over_y, over_y, over_y, over_y,
            over_y, over_y, over_y, over_y, dma((n_ep,)), dma((n_ep,)), over_ep, over_ep,
        ],
        compiler_params=pltpu.CompilerParams(
            collective_id=0, has_side_effects=True, vmem_limit_bytes=62 * 1024 * 1024
        ),
        name="layer",
    )(
        x_path, gate_path, conv_taps, decay_gate_w, input_gate_w, decay_rate, decay_shift.T,
        expert_in, norm_gain.reshape(1, model), routes.T, route_scores.T,
        gate_weight, up_weight, down_weight,
    )
    return hand_over(recurrent, expert)


def solution(mesh):
    in_specs = (
        P("ep", "tp"),
        P("ep", "tp"),
        P(None, "tp"),
        P(None, "tp", None, None),
        P(None, "tp", None, None),
        P(None, "tp"),
        P("ep", "tp"),
        P("ep", None),
        P(),
        P("ep", None),
        P("ep", None),
        P("ep", None, "tp"),
        P("ep", None, "tp"),
        P("ep", "tp", None),
    )
    out_specs = (P("ep", "tp"), P(("ep", "tp"), None))
    return jax.shard_map(local, mesh=mesh, in_specs=in_specs, out_specs=out_specs, check_vma=False)
```
